128 devices in a mesh: ep: 16 (over z, x), tp: 8 (over y, core).
Axes of the slice: x: 4, y: 4, z: 4, core: 2. Of those that a mesh axis runs over, the one named last changes fastest.
Arguments:
- mix_tokens: bfloat16 [32768, 2048], P(('ep', 'tp')), may hold values from -40 to 40
- mix_gain: float32 [2048], replicated, may hold values from 0.1 to 1.9
- query_weight: bfloat16 [2048, 1024], replicated, may hold values from -0.125 to 0.125
- key_weight: bfloat16 [2048, 256], replicated, may hold values from -0.125 to 0.125
- value_weight: bfloat16 [2048, 256], replicated, may hold values from -0.125 to 0.125
- query_gain: float32 [64], replicated, may hold values from 0.5 to 40
- key_gain: float32 [64], replicated, may hold values from 0.1 to 1.9
- sink_logits: float32 [16], replicated, may hold values from 2 to 6
- out_weight: bfloat16 [1024, 2048], replicated, may hold values from -0.1875 to 0.1875
- moe_tokens: bfloat16 [16384, 2048], P(('ep', 'tp')), may hold values from -40 to 40
- moe_gain: float32 [2048], replicated, may hold values from 0.1 to 1.9
- routes: int32 [16384, 2], P(('ep', 'tp')), may hold values from 0 to 15, all different within a row; in each aligned block of 128 rows (0 to 127, 128 to 255, ...) at most 18 rows name the same one
- route_logits: float32 [16384, 2], P(('ep', 'tp')), may hold values from -6 to 6
- gate_weight: bfloat16 [16, 2048, 7168], P('ep', None, 'tp'), may hold values from -0.125 to 0.125
- up_weight: bfloat16 [16, 2048, 7168], P('ep', None, 'tp'), may hold values from -0.125 to 0.125
- down_weight: bfloat16 [16, 7168, 2048], P('ep', 'tp'), may hold values from -0.0625 to 0.0625
Outputs:
- mix_out: bfloat16 [32768, 2048], P(('ep', 'tp'))
- moe_out: bfloat16 [16384, 2048], P(('ep', 'tp'))
The draws below stay inside these ranges and needn't reach their ends.
Inputs may be any that keep to these rules, and one draw needn't show every extreme that they name: `routes`: each row names 2 different experts. Of the rows of one device no expert is named more than 18 times, and in every draw some device names some expert exactly 18 times.
All inputs are finite; a program needn't handle non-finite values.
Results may differ from the reference program's by a relative error of at most 0.015.
The reference program's roundings to bfloat16 on the way count: a program that leaves them out, or rounds other values in their place, can miss the bound.
Values may be sent and summed in bfloat16 or wider, within the bound.
No kernel may reach another device: no remote copies, remote signals or barrier semaphores. Data moves between devices by JAX's collectives and lax.ppermute only.
A program may use at most 128 MiB of HBM per device.

```python
import math
import jax
import jax.numpy as jnp
import numpy as np
from jax import lax

D = 2048
HEADS = 16
KV_HEADS = 4
HEAD_DIM = 64
WINDOW = 128
FF = 7168
TOPK = 2
TOK_MOE = 128
EXPERTS = 16
CAP = 18
TOKENS_MIX = 32768
TOKENS_MOE = 16384
N_EP = 16
N_TP = 8


def activations(key, total_rows):
    first_key, second_key, third_key = jax.random.split(key, 3)
    columns = jnp.exp(jax.random.uniform(second_key, (D,), jnp.float32, -1.2, 1.2))
    scales = jnp.exp(jax.random.uniform(third_key, (total_rows, 1), jnp.float32, -1.2, 1.2))
    base = jax.random.normal(first_key, (total_rows, D), jnp.float32)
    return jnp.clip(base * columns * scales, -40.0, 40.0).astype(jnp.bfloat16)


def draw_mix_tokens(key, part):
    return activations(jax.random.fold_in(key, 11), TOKENS_MIX)


def draw_moe_tokens(key, part):
    return activations(jax.random.fold_in(key, 12), TOKENS_MOE)


def draw_query_gain(key, part):
    inner = jax.random.fold_in(key, 13)
    return jnp.exp(jax.random.uniform(inner, (HEAD_DIM,), jnp.float32, -0.5, 0.5))


def level_of(rng, dims, cuts, low, high):
    gain = 1.0
    for axis_at, parts in cuts:
        steps = jax.random.uniform(jax.random.fold_in(jax.random.fold_in(rng, 6), axis_at), (parts,), jnp.float32, low / len(cuts), high / len(cuts))
        gain = gain * jnp.repeat(jnp.exp(steps), dims[axis_at] // parts).reshape((-1,) + (1,) * (len(dims) - 1 - axis_at))
    return gain


def assign_block(stream_key, own, number, rows, count, top, reach, slope):
    sequence = jax.random.permutation(stream_key, count)
    packed, common = load_shares(count, rows * top, reach, slope, True), load_shares(count, rows * top, reach, slope, False)
    places = jnp.arange(count)

    def named(tallies, offset_by):
        used = int((tallies > 0).sum())
        fixed = max(1, used // 4)
        shifted = fixed + (places - fixed + offset_by * (used - fixed)) % max(1, count - fixed)
        return jnp.zeros((count,), jnp.int32).at[sequence[jnp.where(places < fixed, places, shifted)]].set(jnp.asarray(tallies, jnp.int32))

    tallies = jnp.where(number % 4 == 0, named(packed, number // 4), named(common, number - number // 4 - 1))
    mixed = jax.random.permutation(jax.random.fold_in(own, 3), count)
    donor, sink = mixed[0:count // 2 * 2:2], mixed[1:count // 2 * 2:2]
    margin = jnp.minimum(tallies[donor] - 1, reach - tallies[sink]) // 2
    margin = jnp.where((donor == sequence[0]) | (sink == sequence[0]) | (tallies[sink] == 0), 0, jnp.maximum(margin, 0))
    shifted = jax.random.randint(jax.random.fold_in(own, 4), (count // 2,), 0, 1 << 20) % (margin + 1)
    tallies = tallies.at[donor].add(-shifted).at[sink].add(shifted)
    items = jnp.searchsorted(jnp.cumsum(tallies), jnp.arange(rows * top), side="right").astype(jnp.int32)
    grid = items.reshape(top, rows).T
    grid = grid[jax.random.permutation(jax.random.fold_in(own, 1), rows)]
    offset_by = jax.random.randint(jax.random.fold_in(own, 2), (rows, 1), 0, top)
    return jnp.take_along_axis(grid, (jnp.arange(top)[None, :] + offset_by) % top, axis=1)


def load_shares(count, total, most, skew, full):
    weights = [(1 << 20) // math.isqrt(rank ** skew) + 1 for rank in range(1, count + 1)]
    largest = most if full else min(most, max(-(-total // count), total * weights[0] // sum(weights)))
    least = 1 if total - largest >= count - 1 else 0
    counts, rest = [largest] + [least] * (count - 1), total - largest - least * (count - 1)
    while rest > 0:
        movable = [i for i in range(1, count) if counts[i] < largest] or [i for i in range(1, count) if counts[i] < most]
        whole, remaining = sum([weights[i] for i in movable]), rest
        for i in movable:
            extra = min(most - counts[i], max(1, remaining * weights[i] // whole), rest)
            counts[i] = counts[i] + extra
            rest = rest - extra
    return np.array(counts)


def centred(own_key, dims, width, bound, shards=(), held_as=jnp.bfloat16):
    result = width * jax.random.normal(own_key, dims, jnp.float32)
    if shards:
        result = result * level_of(own_key, dims, shards, -0.22, 0.18)
    return jnp.clip(result, -bound, bound).astype(held_as)


def setup_inputs(seed: int = 0) -> dict:
    keys = jax.random.split(jax.random.key(seed), 17)
    mix_tokens = draw_mix_tokens(jax.random.fold_in(keys[16], 71), 0)
    mix_gain = jnp.clip(1.0 + 0.18 * jax.random.normal(keys[1], (D,), jnp.float32), 0.1, 1.9)
    query_weight = centred(keys[2], (D, HEADS * HEAD_DIM), D ** -0.5, 0.125)
    key_weight = centred(keys[3], (D, KV_HEADS * HEAD_DIM), D ** -0.5, 0.125)
    value_weight = centred(keys[4], (D, KV_HEADS * HEAD_DIM), D ** -0.5, 0.125)
    query_gain = draw_query_gain(jax.random.fold_in(keys[16], 71), 0)
    key_gain = jnp.clip(1.0 + 0.18 * jax.random.normal(keys[6], (HEAD_DIM,), jnp.float32), 0.1, 1.9)
    sink_logits = jnp.clip(jax.random.uniform(keys[7], (HEADS,), jnp.float32, 2.0, 6.0), 2.0, 6.0)
    out_weight = centred(keys[8], (HEADS * HEAD_DIM, D), (HEADS * HEAD_DIM) ** -0.5, 0.1875)
    moe_tokens = draw_moe_tokens(jax.random.fold_in(keys[16], 71), 0)
    moe_gain = jnp.clip(1.0 + 0.18 * jax.random.normal(keys[10], (D,), jnp.float32), 0.1, 1.9)
    routes_keys = jax.random.split(jax.random.fold_in(keys[11], 1), TOKENS_MOE // TOK_MOE)
    routes_turns = jax.random.permutation(jax.random.fold_in(keys[11], 3), TOKENS_MOE // TOK_MOE)
    routes = jax.vmap(lambda own, number: assign_block(jax.random.fold_in(keys[11], 2), own, number, TOK_MOE, EXPERTS, TOPK, CAP, 0))(routes_keys, routes_turns).reshape((TOKENS_MOE, TOPK))
    route_logits = centred(keys[12], (TOKENS_MOE, TOPK), 1.5, 6.0, ((0, 128),), jnp.float32)
    gate_weight = centred(keys[13], (EXPERTS, D, FF), D ** -0.5, 0.125, ((0, 16), (2, 8)))
    up_weight = centred(keys[14], (EXPERTS, D, FF), D ** -0.5, 0.125, ((0, 16), (2, 8)))
    down_weight = centred(keys[15], (EXPERTS, FF, D), FF ** -0.5, 0.0625, ((0, 16), (1, 8)))
    return {"mix_tokens": mix_tokens, "mix_gain": mix_gain, "query_weight": query_weight, "key_weight": key_weight, "value_weight": value_weight, "query_gain": query_gain, "key_gain": key_gain, "sink_logits": sink_logits, "out_weight": out_weight, "moe_tokens": moe_tokens, "moe_gain": moe_gain, "routes": routes, "route_logits": route_logits, "gate_weight": gate_weight, "up_weight": up_weight, "down_weight": down_weight}


epsilon = 1e-06

def rms_scale(values, gain_vec):
    values = values.astype(jnp.float32)
    return values * lax.rsqrt(lax.optimization_barrier(jnp.mean(values * values, axis=-1, keepdims=True)) + epsilon) * gain_vec

def route_slots(routes, experts, capacity):
    flat_ids = routes.reshape(-1)
    onehot = (flat_ids[:, None] == jnp.arange(experts, dtype=jnp.int32)[None, :]).astype(jnp.int32)
    before = jnp.cumsum(onehot, axis=0) - onehot
    slot_ids = lax.optimization_barrier(jnp.sum(before * onehot, axis=1))
    return (flat_ids * capacity + slot_ids).reshape(routes.shape).astype(jnp.int32)

def window_attention(queries, key_ext, value_ext, sink_logits, first_pos):
    row_count = queries.shape[0]
    window_rows = key_ext.shape[0] - row_count
    blocks = row_count // window_rows
    kv_heads = key_ext.shape[1]
    group_size = queries.shape[1] // kv_heads
    head_dim = queries.shape[2]
    query_blk = queries.reshape(blocks, window_rows, kv_heads, group_size, head_dim)

    def pair_up(source):
        lower = source[:row_count].reshape(blocks, window_rows, kv_heads, head_dim)
        upper = source[window_rows:].reshape(blocks, window_rows, kv_heads, head_dim)
        return jnp.concatenate([lower, upper], axis=1)
    key_blk = pair_up(key_ext)
    value_blk = pair_up(value_ext)
    scores = jnp.einsum('bqkgd,bskd->bkgqs', query_blk.astype(jnp.float32), key_blk.astype(jnp.float32)) * head_dim ** (-0.5)
    query_pos = jnp.arange(window_rows, dtype=jnp.int32)[:, None] + window_rows
    key_pos = jnp.arange(2 * window_rows, dtype=jnp.int32)[None, :]
    pos_gap = query_pos - key_pos
    block_start = first_pos + jnp.arange(blocks, dtype=jnp.int32) * window_rows - window_rows
    key_global = block_start[:, None] + jnp.arange(2 * window_rows, dtype=jnp.int32)[None, :]
    visible = ((pos_gap >= 0) & (pos_gap <= window_rows))[None] & (key_global >= 0)[:, None, :]
    scores = jnp.where(visible[:, None, None], scores, -jnp.inf)
    sink_col = sink_logits.astype(jnp.float32).reshape(kv_heads, group_size)[None, :, :, None, None]
    row_top = jnp.maximum(lax.optimization_barrier(jnp.max(scores, axis=-1, keepdims=True)), sink_col)
    weights = jnp.exp(scores - row_top)
    denom_sum = lax.optimization_barrier(jnp.sum(weights, axis=-1, keepdims=True)) + jnp.exp(sink_col - row_top)
    attn_prob = (weights / denom_sum).astype(jnp.bfloat16)
    mixed_out = jnp.einsum('bkgqs,bskd->bqkgd', attn_prob.astype(jnp.float32), value_blk.astype(jnp.float32))
    return mixed_out.astype(jnp.bfloat16).reshape(row_count, -1)

def reference(mix_tokens, mix_gain, query_weight, key_weight, value_weight, query_gain, key_gain, sink_logits, out_weight, moe_tokens, moe_gain, routes, route_logits, gate_weight, up_weight, down_weight):
    total_rows = mix_tokens.shape[0]
    normed = rms_scale(mix_tokens, mix_gain).astype(jnp.bfloat16)
    queries = jnp.dot(normed, query_weight, preferred_element_type=jnp.float32)
    queries = rms_scale(queries.reshape(total_rows, HEADS, HEAD_DIM), query_gain).astype(jnp.bfloat16)
    key_rows = jnp.dot(normed, key_weight, preferred_element_type=jnp.float32)
    key_rows = rms_scale(key_rows.reshape(total_rows, KV_HEADS, HEAD_DIM), key_gain).astype(jnp.bfloat16)
    values = jnp.dot(normed, value_weight, preferred_element_type=jnp.float32).astype(jnp.bfloat16)
    values = values.reshape(total_rows, KV_HEADS, HEAD_DIM)
    zero_rim = jnp.zeros((WINDOW, KV_HEADS, HEAD_DIM), jnp.bfloat16)
    key_ext = jnp.concatenate([zero_rim, key_rows], axis=0)
    value_ext = jnp.concatenate([zero_rim, values], axis=0)

    def one_block(block_index):
        first_row = (block_index * WINDOW).astype(jnp.int32)
        query_part = lax.dynamic_slice_in_dim(queries, first_row, WINDOW, 0)
        key_part = lax.dynamic_slice_in_dim(key_ext, first_row, 2 * WINDOW, 0)
        value_part = lax.dynamic_slice_in_dim(value_ext, first_row, 2 * WINDOW, 0)
        return window_attention(query_part, key_part, value_part, sink_logits, first_row)
    attended = lax.map(one_block, jnp.arange(total_rows // WINDOW, dtype=jnp.int32))
    attended = attended.reshape(total_rows, HEADS * HEAD_DIM)
    mix_out = jnp.dot(attended, out_weight, preferred_element_type=jnp.float32).astype(jnp.bfloat16)
    devices = N_EP * N_TP
    experts = N_EP
    moe_normed = rms_scale(moe_tokens, moe_gain).astype(jnp.bfloat16)
    targets = jax.vmap(lambda block_routes: route_slots(block_routes, experts, CAP))(routes.reshape(devices, TOK_MOE, TOPK))
    expert_of = targets // CAP
    slot_of = targets - expert_of * CAP
    device_of = jnp.arange(devices, dtype=jnp.int32)[:, None, None]
    slot_pos = expert_of * (devices * CAP) + device_of * CAP + slot_of
    token_index = device_of * TOK_MOE + jnp.arange(TOK_MOE, dtype=jnp.int32)[None, :, None] + 0 * slot_of
    slot_table = jnp.zeros((experts * devices * CAP,), jnp.int32).at[slot_pos.reshape(-1)].set(token_index.reshape(-1))
    slot_table = slot_table.reshape(experts, devices * CAP)
    group_width = FF // N_TP

    def one_expert(expert_args):
        table_row, gate_mat, up_mat, down_mat = expert_args
        inputs = moe_normed[table_row]
        summed = jnp.zeros((inputs.shape[0], D), jnp.float32)
        for shard_index in range(N_TP):
            low = shard_index * group_width
            gate_act = jnp.dot(inputs, gate_mat[:, low:low + group_width], preferred_element_type=jnp.float32)
            up_act = jnp.dot(inputs, up_mat[:, low:low + group_width], preferred_element_type=jnp.float32)
            hidden = (jax.nn.silu(gate_act) * up_act).astype(jnp.bfloat16)
            partial_value = jnp.dot(hidden, down_mat[low:low + group_width], preferred_element_type=jnp.float32).astype(jnp.bfloat16)
            summed = summed + partial_value.astype(jnp.float32)
        return summed.astype(jnp.bfloat16)
    expert_out = lax.map(one_expert, (slot_table, gate_weight, up_weight, down_weight))
    picked = expert_out.reshape(-1, D)[slot_pos.reshape(TOKENS_MOE, TOPK)]
    gate_probs = jax.nn.softmax(route_logits.astype(jnp.float32), axis=-1).astype(jnp.bfloat16)
    moe_out = lax.optimization_barrier(jnp.sum(gate_probs.astype(jnp.float32)[:, :, None] * picked.astype(jnp.float32), axis=1)).astype(jnp.bfloat16)
    return (mix_out, moe_out)
```

```python
import jax
import jax.numpy as jnp
from jax import lax
from jax.sharding import PartitionSpec as P

WINDOW = 128
CORES = 2


epsilon = 1e-06
AXES = ("ep", "tp")


def passed_along(block, axis, distance):
    devices = range(lax.axis_size(axis))
    route = [(i - distance, i) for i in devices if i - distance in devices]
    return lax.ppermute(block, axis, route)


def chip_shift(block, distance):
    size = lax.axis_size("tp")
    route = [(i, (i + CORES * distance) % size) for i in range(size)]
    return lax.ppermute(block, "tp", route)


def core_swap(block):
    route = [(i, i ^ 1) for i in range(lax.axis_size("tp"))]
    return lax.ppermute(block, "tp", route)


def rms_scale(values, gain_vec):
    values = values.astype(jnp.float32)
    return (
        values * lax.rsqrt(jnp.mean(values * values, axis=-1, keepdims=True) + epsilon) * gain_vec
    )


def route_slots(routes, experts, capacity):
    flat_ids = routes.reshape(-1)
    onehot = (flat_ids[:, None] == jnp.arange(experts, dtype=jnp.int32)[None, :]).astype(jnp.int32)
    before = jnp.cumsum(onehot, axis=0) - onehot
    slot_ids = jnp.sum(before * onehot, axis=1)
    return (flat_ids * capacity + slot_ids).reshape(routes.shape)


def window_attention(queries, key_ext, value_ext, sink_logits, first_pos):
    row_count = queries.shape[0]
    window_rows = key_ext.shape[0] - row_count
    blocks = row_count // window_rows
    kv_heads = key_ext.shape[1]
    group_size = queries.shape[1] // kv_heads
    head_dim = queries.shape[2]
    query_blk = queries.reshape(blocks, window_rows, kv_heads, group_size, head_dim)

    def pair_up(source):
        lower = source[:row_count].reshape(blocks, window_rows, kv_heads, head_dim)
        upper = source[window_rows:].reshape(blocks, window_rows, kv_heads, head_dim)
        return jnp.concatenate([lower, upper], axis=1)

    key_blk = pair_up(key_ext)
    value_blk = pair_up(value_ext)
    scores = jnp.einsum(
        "bqkgd,bskd->bkgqs", query_blk, key_blk, preferred_element_type=jnp.float32
    ) * head_dim ** (-0.5)
    query_pos = jnp.arange(window_rows, dtype=jnp.int32)[:, None] + window_rows
    key_pos = jnp.arange(2 * window_rows, dtype=jnp.int32)[None, :]
    pos_gap = query_pos - key_pos
    block_start = first_pos + jnp.arange(blocks, dtype=jnp.int32) * window_rows - window_rows
    key_global = block_start[:, None] + jnp.arange(2 * window_rows, dtype=jnp.int32)[None, :]
    visible = ((pos_gap >= 0) & (pos_gap <= window_rows))[None] & (key_global >= 0)[:, None, :]
    scores = jnp.where(visible[:, None, None], scores, -jnp.inf)
    sink_col = sink_logits.reshape(kv_heads, group_size)[None, :, :, None, None]
    row_top = jnp.maximum(jnp.max(scores, axis=-1, keepdims=True), sink_col)
    weights = jnp.exp(scores - row_top)
    denom_sum = jnp.sum(weights, axis=-1, keepdims=True) + jnp.exp(sink_col - row_top)
    attn_prob = (weights / denom_sum).astype(jnp.bfloat16)
    mixed_out = jnp.einsum(
        "bkgqs,bskd->bqkgd", attn_prob, value_blk, preferred_element_type=jnp.float32
    )
    return mixed_out.astype(jnp.bfloat16).reshape(row_count, -1)


def attention(
    mix_tokens,
    mix_gain,
    query_weight,
    key_weight,
    value_weight,
    query_gain,
    key_gain,
    sink_logits,
    out_weight,
):
    row_count = mix_tokens.shape[0]
    head_count = sink_logits.shape[0]
    head_dim = query_gain.shape[0]
    kv_heads = key_weight.shape[1] // head_dim
    normed = rms_scale(mix_tokens, mix_gain).astype(jnp.bfloat16)
    queries = jnp.dot(normed, query_weight, preferred_element_type=jnp.float32)
    queries = rms_scale(queries.reshape(row_count, head_count, head_dim), query_gain).astype(
        jnp.bfloat16
    )
    key_rows = jnp.dot(normed, key_weight, preferred_element_type=jnp.float32)
    key_rows = rms_scale(key_rows.reshape(row_count, kv_heads, head_dim), key_gain).astype(
        jnp.bfloat16
    )
    values = jnp.dot(normed, value_weight, preferred_element_type=jnp.float32).astype(jnp.bfloat16)
    values = values.reshape(row_count, kv_heads, head_dim)
    rim_keys, rim_values = passed_along(
        (key_rows[row_count - WINDOW :], values[row_count - WINDOW :]), ("ep", "tp"), 1
    )
    key_ext = jnp.concatenate([rim_keys, key_rows], axis=0)
    value_ext = jnp.concatenate([rim_values, values], axis=0)
    first_pos = lax.axis_index(("ep", "tp")) * row_count
    attended = window_attention(queries, key_ext, value_ext, sink_logits, first_pos)
    return jnp.dot(attended, out_weight, preferred_element_type=jnp.float32).astype(jnp.bfloat16)


def expert_partial(rows, gate_mat, up_mat, down_mat):
    gate_act = jnp.dot(rows, gate_mat, preferred_element_type=jnp.float32)
    up_act = jnp.dot(rows, up_mat, preferred_element_type=jnp.float32)
    hidden = (jax.nn.silu(gate_act) * up_act).astype(jnp.bfloat16)
    return jnp.dot(hidden, down_mat, preferred_element_type=jnp.float32).astype(jnp.bfloat16)


def exchange(rows, experts):
    count, width = rows.shape
    lanes = 128
    view = rows.reshape(experts, count * width // (experts * lanes), lanes)
    view = lax.all_to_all(view, "ep", split_axis=0, concat_axis=0, tiled=True)
    return view.reshape(count, width)


def body(
    mix_tokens,
    mix_gain,
    query_weight,
    key_weight,
    value_weight,
    query_gain,
    key_gain,
    sink_logits,
    out_weight,
    moe_tokens,
    moe_gain,
    routes,
    route_logits,
    gate_weight,
    up_weight,
    down_weight,
):
    mix_out = attention(
        mix_tokens,
        mix_gain,
        query_weight,
        key_weight,
        value_weight,
        query_gain,
        key_gain,
        sink_logits,
        out_weight,
    )
    moe_rows = moe_tokens.shape[0]
    experts = lax.axis_size("ep")
    capacity = (9 * moe_rows * routes.shape[1] + 8 * experts - 1) // (8 * experts)
    moe_normed = rms_scale(moe_tokens, moe_gain).astype(jnp.bfloat16)
    targets = route_slots(routes, experts, capacity)
    slot_ids = jnp.arange(experts * capacity, dtype=jnp.int32)
    pick_rows = jnp.sum(
        (targets[None, :, :] == slot_ids[:, None, None]).astype(jnp.bfloat16), axis=2
    )
    packed = jnp.dot(pick_rows, moe_normed, preferred_element_type=jnp.float32).astype(jnp.bfloat16)
    own = exchange(packed, experts)

    far = chip_shift(own, 2)
    after = chip_shift(own, 1)
    before = chip_shift(own, -1)

    def both_cores(block):
        other = core_swap(block)
        rows = jnp.concatenate([block, other], axis=0)
        part = expert_partial(rows, gate_weight[0], up_weight[0], down_weight[0])
        count = block.shape[0]
        theirs = core_swap(part[count:])
        return part[:count].astype(jnp.float32) + theirs.astype(jnp.float32)

    total = both_cores(own)
    far_sum = chip_shift(both_cores(far).astype(jnp.bfloat16), 2)
    after_sum = chip_shift(both_cores(after).astype(jnp.bfloat16), -1)
    before_sum = chip_shift(both_cores(before).astype(jnp.bfloat16), 1)
    total = (
        total
        + far_sum.astype(jnp.float32)
        + after_sum.astype(jnp.float32)
        + before_sum.astype(jnp.float32)
    )
    results = exchange(total.astype(jnp.bfloat16), experts)

    gate_probs = jax.nn.softmax(route_logits, axis=-1).astype(jnp.bfloat16)
    combine = jnp.where(
        targets[:, :, None] == slot_ids[None, None, :],
        gate_probs[:, :, None],
        jnp.zeros((), jnp.bfloat16),
    )
    combine = jnp.sum(combine, axis=1)
    moe_out = jnp.dot(combine, results, preferred_element_type=jnp.float32).astype(jnp.bfloat16)
    return (mix_out, moe_out)


def solution(mesh):
    placed = (
        P(("ep", "tp"), None),
        P(),
        P(),
        P(),
        P(),
        P(),
        P(),
        P(),
        P(),
        P(("ep", "tp"), None),
        P(),
        P(("ep", "tp"), None),
        P(("ep", "tp"), None),
        P("ep", None, "tp"),
        P("ep", None, "tp"),
        P("ep", "tp", None),
    )
    return jax.shard_map(
        body,
        mesh=mesh,
        in_specs=placed,
        out_specs=(P(("ep", "tp"), None), P(("ep", "tp"), None)),
        check_vma=False,
    )
```

```python
import functools

import jax
import jax.numpy as jnp
from jax import lax
from jax.experimental import pallas as pl
from jax.experimental.pallas import tpu as pltpu
from jax.sharding import PartitionSpec as P

WINDOW = 128
CORES = 2


epsilon = 1e-06


def passed_along(block, axis, distance):
    devices = range(lax.axis_size(axis))
    route = [(i - distance, i) for i in devices if i - distance in devices]
    return lax.ppermute(block, axis, route)


def outward(block, distance):
    size = lax.axis_size("tp")
    route = [(i, (i + CORES * distance * (1 - 2 * (i % CORES))) % size) for i in range(size)]
    return lax.ppermute(block, "tp", route)


def core_swap(block):
    route = [(i, i ^ 1) for i in range(lax.axis_size("tp"))]
    return lax.ppermute(block, "tp", route)


def rms_scale(values, gain_vec):
    values = values.astype(jnp.float32)
    return (
        values * lax.rsqrt(jnp.mean(values * values, axis=-1, keepdims=True) + epsilon) * gain_vec
    )


def route_slots(routes, experts, capacity):
    flat_ids = routes.reshape(-1)
    onehot = (flat_ids[:, None] == jnp.arange(experts, dtype=jnp.int32)[None, :]).astype(jnp.int32)
    before = jnp.cumsum(onehot, axis=0) - onehot
    slot_ids = jnp.sum(before * onehot, axis=1)
    return (flat_ids * capacity + slot_ids).reshape(routes.shape)


def window_attention(queries, key_ext, value_ext, sink_logits, first_pos):
    row_count = queries.shape[0]
    window_rows = key_ext.shape[0] - row_count
    blocks = row_count // window_rows
    kv_heads = key_ext.shape[1]
    group_size = queries.shape[1] // kv_heads
    head_dim = queries.shape[2]
    query_blk = queries.reshape(blocks, window_rows, kv_heads, group_size, head_dim)

    def pair_up(source):
        lower = source[:row_count].reshape(blocks, window_rows, kv_heads, head_dim)
        upper = source[window_rows:].reshape(blocks, window_rows, kv_heads, head_dim)
        return jnp.concatenate([lower, upper], axis=1)

    key_blk = pair_up(key_ext)
    value_blk = pair_up(value_ext)
    scores = jnp.einsum(
        "bqkgd,bskd->bkgqs", query_blk, key_blk, preferred_element_type=jnp.float32
    ) * head_dim ** (-0.5)
    query_pos = jnp.arange(window_rows, dtype=jnp.int32)[:, None] + window_rows
    key_pos = jnp.arange(2 * window_rows, dtype=jnp.int32)[None, :]
    pos_gap = query_pos - key_pos
    block_start = first_pos + jnp.arange(blocks, dtype=jnp.int32) * window_rows - window_rows
    key_global = block_start[:, None] + jnp.arange(2 * window_rows, dtype=jnp.int32)[None, :]
    visible = ((pos_gap >= 0) & (pos_gap <= window_rows))[None] & (key_global >= 0)[:, None, :]
    scores = jnp.where(visible[:, None, None], scores, -jnp.inf)
    sink_col = sink_logits.reshape(kv_heads, group_size)[None, :, :, None, None]
    row_top = jnp.maximum(jnp.max(scores, axis=-1, keepdims=True), sink_col)
    weights = jnp.exp(scores - row_top)
    denom_sum = jnp.sum(weights, axis=-1, keepdims=True) + jnp.exp(sink_col - row_top)
    attn_prob = (weights / denom_sum).astype(jnp.bfloat16)
    mixed_out = jnp.einsum(
        "bkgqs,bskd->bqkgd", attn_prob, value_blk, preferred_element_type=jnp.float32
    )
    return mixed_out.astype(jnp.bfloat16).reshape(row_count, -1)


def attention(
    mix_tokens,
    mix_gain,
    query_weight,
    key_weight,
    value_weight,
    query_gain,
    key_gain,
    sink_logits,
    out_weight,
):
    row_count = mix_tokens.shape[0]
    head_count = sink_logits.shape[0]
    head_dim = query_gain.shape[0]
    kv_heads = key_weight.shape[1] // head_dim
    normed = rms_scale(mix_tokens, mix_gain).astype(jnp.bfloat16)
    key_rows = jnp.dot(normed, key_weight, preferred_element_type=jnp.float32)
    key_rows = rms_scale(key_rows.reshape(row_count, kv_heads, head_dim), key_gain).astype(
        jnp.bfloat16
    )
    values = jnp.dot(normed, value_weight, preferred_element_type=jnp.float32).astype(jnp.bfloat16)
    values = values.reshape(row_count, kv_heads, head_dim)
    edge = jnp.concatenate([key_rows[row_count - WINDOW :], values[row_count - WINDOW :]], axis=1)
    rim = passed_along(edge, ("ep", "tp"), 1)
    rim_keys, rim_values = rim[:, :kv_heads], rim[:, kv_heads:]
    queries = jnp.dot(normed, query_weight, preferred_element_type=jnp.float32)
    queries = rms_scale(queries.reshape(row_count, head_count, head_dim), query_gain).astype(
        jnp.bfloat16
    )
    key_ext = jnp.concatenate([rim_keys, key_rows], axis=0)
    value_ext = jnp.concatenate([rim_values, values], axis=0)
    first_pos = lax.axis_index(("ep", "tp")) * row_count
    attended = window_attention(queries, key_ext, value_ext, sink_logits, first_pos)
    return jnp.dot(attended, out_weight, preferred_element_type=jnp.float32).astype(jnp.bfloat16)


def expert_kernel(count, *refs):
    rows = refs[:count]
    gate_ref, up_ref, down_ref = refs[count : count + 3]
    outs = refs[count + 3 : 2 * count + 3]
    first, second, hidden, sems = refs[2 * count + 3 :]
    inner = gate_ref.shape[1]
    half = down_ref.shape[1] // 2
    cuts = ((0, 512), (512, inner - 512))
    copies = []
    for n, (low, size) in enumerate(cuts):
        for m, source in enumerate((gate_ref, up_ref)):
            copies.append(
                pltpu.make_async_copy(
                    source.at[:, pl.ds(low, size)],
                    first.at[:, pl.ds(2 * low + m * size, size)],
                    sems.at[2 * n + m],
                )
            )
    for n in range(2):
        part = pl.ds(half * n, half)
        copies.append(
            pltpu.make_async_copy(down_ref.at[:, part], second.at[:, part], sems.at[4 + n])
        )
    for copy in copies:
        copy.start()
    for n, (low, size) in enumerate(cuts):
        copies[2 * n].wait()
        copies[2 * n + 1].wait()
        for k in range(count):
            act = jnp.dot(
                rows[k][...],
                first[:, 2 * low : 2 * low + 2 * size],
                preferred_element_type=jnp.float32,
            )
            gate_act = act[:, :size]
            hidden[k, :, low : low + size] = (
                gate_act * jax.nn.sigmoid(gate_act) * act[:, size:]
            ).astype(jnp.bfloat16)
    for n in range(2):
        copies[4 + n].wait()
        for k in range(count):
            outs[k][:, half * n : half * n + half] = jnp.dot(
                hidden[k],
                second[:, half * n : half * n + half],
                preferred_element_type=jnp.float32,
            ).astype(jnp.bfloat16)


def expert_partial(blocks, gate_mat, up_mat, down_mat):
    count = len(blocks)
    rows, width = blocks[0].shape
    inner = gate_mat.shape[1]
    near = pl.BlockSpec(memory_space=pltpu.VMEM)
    far = pl.BlockSpec(memory_space=pltpu.HBM)
    return pl.pallas_call(
        functools.partial(expert_kernel, count),
        out_shape=[jax.ShapeDtypeStruct((rows, width), jnp.bfloat16)] * count,
        in_specs=[near] * count + [far] * 3,
        out_specs=[near] * count,
        scratch_shapes=[
            pltpu.VMEM((width, 2 * inner), jnp.bfloat16),
            pltpu.VMEM((inner, width), jnp.bfloat16),
            pltpu.VMEM((count, rows, inner), jnp.bfloat16),
            pltpu.SemaphoreType.DMA((6,)),
        ],
        compiler_params=pltpu.CompilerParams(vmem_limit_bytes=44 << 20),
        cost_estimate=pl.CostEstimate(
            flops=6 * count * rows * width * inner,
            transcendentals=count * rows * inner,
            bytes_accessed=2 * (3 * width * inner + 2 * count * rows * width),
        ),
    )(*blocks, gate_mat, up_mat, down_mat)


def added(*parts):
    return sum(part.astype(jnp.float32) for part in parts).astype(jnp.bfloat16)


def exchange(rows, experts):
    count, width = rows.shape
    lanes = 128
    view = rows.reshape(experts, count * width // (experts * lanes), lanes)
    view = lax.all_to_all(view, "ep", split_axis=0, concat_axis=0, tiled=True)
    return view.reshape(count, width)


def body(
    mix_tokens,
    mix_gain,
    query_weight,
    key_weight,
    value_weight,
    query_gain,
    key_gain,
    sink_logits,
    out_weight,
    moe_tokens,
    moe_gain,
    routes,
    route_logits,
    gate_weight,
    up_weight,
    down_weight,
):
    mix_out = attention(
        mix_tokens,
        mix_gain,
        query_weight,
        key_weight,
        value_weight,
        query_gain,
        key_gain,
        sink_logits,
        out_weight,
    )
    moe_rows = moe_tokens.shape[0]
    experts = lax.axis_size("ep")
    capacity = (9 * moe_rows * routes.shape[1] + 8 * experts - 1) // (8 * experts)
    moe_normed = rms_scale(moe_tokens, moe_gain).astype(jnp.bfloat16)
    targets = route_slots(routes, experts, capacity)
    slot_ids = jnp.arange(experts * capacity, dtype=jnp.int32)
    pick_rows = jnp.sum(
        (targets[None, :, :] == slot_ids[:, None, None]).astype(jnp.bfloat16), axis=2
    )
    packed = jnp.dot(pick_rows, moe_normed, preferred_element_type=jnp.float32).astype(jnp.bfloat16)
    own = exchange(packed, experts)

    def run(blocks):
        return expert_partial(blocks, gate_weight[0], up_weight[0], down_weight[0])

    near_a = outward(own, 1)
    own_b = core_swap(own)
    near_b = outward(own_b, 1)
    far_a = outward(near_a, 1)
    across_b = core_swap(near_a)
    across_a = core_swap(near_b)
    far_b = core_swap(far_a)

    own_part_a, own_part_b = run([own, own_b])
    near_part_a, across_part_b = run([near_a, across_b])
    near_part_b, across_part_a = run([near_b, across_a])
    far_part_a, far_part_b = run([far_a, far_b])

    back_a = added(near_part_a, core_swap(across_part_b))
    back_b = added(near_part_b, core_swap(across_part_a))
    far_sum = added(far_part_a, core_swap(far_part_b))
    home_b = outward(back_b, -1)
    passing = outward(far_sum, -1)
    home_a = outward(added(back_a, passing), -1)
    crossing = core_swap(added(own_part_b, home_b))
    total = added(own_part_a, home_a, crossing)
    results = exchange(total, experts)

    gate_probs = jax.nn.softmax(route_logits, axis=-1).astype(jnp.bfloat16)
    combine = jnp.where(
        targets[:, :, None] == slot_ids[None, None, :],
        gate_probs[:, :, None],
        jnp.zeros((), jnp.bfloat16),
    )
    combine = jnp.sum(combine, axis=1)
    moe_out = jnp.dot(combine, results, preferred_element_type=jnp.float32).astype(jnp.bfloat16)
    return (mix_out, moe_out)


def solution(mesh):
    placed = (
        P(("ep", "tp"), None),
        P(),
        P(),
        P(),
        P(),
        P(),
        P(),
        P(),
        P(),
        P(("ep", "tp"), None),
        P(),
        P(("ep", "tp"), None),
        P(("ep", "tp"), None),
        P("ep", None, "tp"),
        P("ep", None, "tp"),
        P("ep", "tp", None),
    )

    return jax.shard_map(
        body,
        mesh=mesh,
        in_specs=placed,
        out_specs=(P(("ep", "tp"), None), P(("ep", "tp"), None)),
        check_vma=False,
    )
```

```python
import functools

import jax
import jax.numpy as jnp
from jax import lax
from jax.experimental import pallas as pl
from jax.experimental.pallas import tpu as pltpu
from jax.sharding import PartitionSpec as P

WINDOW = 128
CORES = 2
TILE = 512


epsilon = 1e-06


def passed_along(block, axis, distance):
    devices = range(lax.axis_size(axis))
    route = [(i - distance, i) for i in devices if i - distance in devices]
    return lax.ppermute(block, axis, route)


def outward(block, distance):
    size = lax.axis_size("tp")
    route = [(i, (i + CORES * distance * (1 - 2 * (i % CORES))) % size) for i in range(size)]
    return lax.ppermute(block, "tp", route)


def core_swap(block):
    route = [(i, i ^ 1) for i in range(lax.axis_size("tp"))]
    return lax.ppermute(block, "tp", route)


def rms_scale(values, gain_vec):
    values = values.astype(jnp.float32)
    return (
        values * lax.rsqrt(jnp.mean(values * values, axis=-1, keepdims=True) + epsilon) * gain_vec
    )


def route_slots(routes, experts, capacity):
    flat_ids = routes.reshape(-1)
    onehot = (flat_ids[:, None] == jnp.arange(experts, dtype=jnp.int32)[None, :]).astype(jnp.int32)
    before = jnp.cumsum(onehot, axis=0) - onehot
    slot_ids = jnp.sum(before * onehot, axis=1)
    return (flat_ids * capacity + slot_ids).reshape(routes.shape)


def window_attention(queries, key_ext, value_ext, sink_logits, first_pos):
    row_count = queries.shape[0]
    window_rows = key_ext.shape[0] - row_count
    blocks = row_count // window_rows
    kv_heads = key_ext.shape[1]
    group_size = queries.shape[1] // kv_heads
    head_dim = queries.shape[2]
    query_blk = queries.reshape(blocks, window_rows, kv_heads, group_size, head_dim)

    def pair_up(source):
        lower = source[:row_count].reshape(blocks, window_rows, kv_heads, head_dim)
        upper = source[window_rows:].reshape(blocks, window_rows, kv_heads, head_dim)
        return jnp.concatenate([lower, upper], axis=1)

    key_blk = pair_up(key_ext)
    value_blk = pair_up(value_ext)
    scores = jnp.einsum(
        "bqkgd,bskd->bkgqs", query_blk, key_blk, preferred_element_type=jnp.float32
    ) * head_dim ** (-0.5)
    query_pos = jnp.arange(window_rows, dtype=jnp.int32)[:, None] + window_rows
    key_pos = jnp.arange(2 * window_rows, dtype=jnp.int32)[None, :]
    pos_gap = query_pos - key_pos
    block_start = first_pos + jnp.arange(blocks, dtype=jnp.int32) * window_rows - window_rows
    key_global = block_start[:, None] + jnp.arange(2 * window_rows, dtype=jnp.int32)[None, :]
    visible = ((pos_gap >= 0) & (pos_gap <= window_rows))[None] & (key_global >= 0)[:, None, :]
    scores = jnp.where(visible[:, None, None], scores, -jnp.inf)
    sink_col = sink_logits.reshape(kv_heads, group_size)[None, :, :, None, None]
    row_top = jnp.maximum(jnp.max(scores, axis=-1, keepdims=True), sink_col)
    weights = jnp.exp(scores - row_top)
    denom_sum = jnp.sum(weights, axis=-1, keepdims=True) + jnp.exp(sink_col - row_top)
    attn_prob = (weights / denom_sum).astype(jnp.bfloat16)
    mixed_out = jnp.einsum(
        "bkgqs,bskd->bqkgd", attn_prob, value_blk, preferred_element_type=jnp.float32
    )
    return mixed_out.astype(jnp.bfloat16).reshape(row_count, -1)


def attention(
    mix_tokens,
    mix_gain,
    query_weight,
    key_weight,
    value_weight,
    query_gain,
    key_gain,
    sink_logits,
    out_weight,
):
    row_count = mix_tokens.shape[0]
    head_count = sink_logits.shape[0]
    head_dim = query_gain.shape[0]
    kv_heads = key_weight.shape[1] // head_dim
    normed = rms_scale(mix_tokens, mix_gain).astype(jnp.bfloat16)
    key_rows = jnp.dot(normed, key_weight, preferred_element_type=jnp.float32)
    key_rows = rms_scale(key_rows.reshape(row_count, kv_heads, head_dim), key_gain).astype(
        jnp.bfloat16
    )
    values = jnp.dot(normed, value_weight, preferred_element_type=jnp.float32).astype(
        jnp.bfloat16
    )
    values = values.reshape(row_count, kv_heads, head_dim)
    edge = jnp.concatenate([key_rows[row_count - WINDOW :], values[row_count - WINDOW :]], axis=1)
    rim = passed_along(edge, ("ep", "tp"), 1)
    rim_keys, rim_values = rim[:, :kv_heads], rim[:, kv_heads:]
    queries = jnp.dot(normed, query_weight, preferred_element_type=jnp.float32)
    queries = rms_scale(queries.reshape(row_count, head_count, head_dim), query_gain).astype(
        jnp.bfloat16
    )
    key_ext = jnp.concatenate([rim_keys, key_rows], axis=0)
    value_ext = jnp.concatenate([rim_values, values], axis=0)
    first_pos = lax.axis_index(("ep", "tp")) * row_count
    attended = window_attention(queries, key_ext, value_ext, sink_logits, first_pos)
    return jnp.dot(attended, out_weight, preferred_element_type=jnp.float32).astype(
        jnp.bfloat16
    )


def expert_kernel(count, *refs):
    rows = refs[:count]
    gate_ref, up_ref, down_ref = refs[count : count + 3]
    outs = refs[count + 3 : 2 * count + 3]
    stacked, hidden = refs[2 * count + 3 :]
    inner = gate_ref.shape[1]
    for k in range(count):
        stacked[k] = rows[k][...]

    @pl.loop(0, count)
    def _(k):
        block = stacked[k]
        for low in range(0, inner, TILE):
            cut = slice(low, min(low + TILE, inner))
            gate_act = jnp.dot(block, gate_ref[:, cut], preferred_element_type=jnp.float32)
            up_act = jnp.dot(block, up_ref[:, cut], preferred_element_type=jnp.float32)
            hidden[k, :, cut] = (gate_act * jax.nn.sigmoid(gate_act) * up_act).astype(
                jnp.bfloat16
            )

    @pl.loop(0, down_ref.shape[1] // TILE)
    def _(index):
        cut = pl.ds(pl.multiple_of(index * TILE, TILE), TILE)
        for k in range(count):
            outs[k][:, cut] = jnp.dot(
                hidden[k], down_ref[:, cut], preferred_element_type=jnp.float32
            ).astype(jnp.bfloat16)


def expert_partial(blocks, gate_mat, up_mat, down_mat):
    count = len(blocks)
    rows, width = blocks[0].shape
    inner = gate_mat.shape[1]
    near = pl.BlockSpec(memory_space=pltpu.VMEM)
    return pl.pallas_call(
        functools.partial(expert_kernel, count),
        out_shape=[jax.ShapeDtypeStruct((rows, width), jnp.bfloat16)] * count,
        in_specs=[near] * (count + 3),
        out_specs=[near] * count,
        scratch_shapes=[
            pltpu.VMEM((count, rows, width), jnp.bfloat16),
            pltpu.VMEM((count, rows, inner), jnp.bfloat16),
        ],
        compiler_params=pltpu.CompilerParams(vmem_limit_bytes=24 << 20),
        cost_estimate=pl.CostEstimate(
            flops=6 * count * rows * width * inner,
            transcendentals=count * rows * inner,
            bytes_accessed=2 * (3 * width * inner + 2 * count * rows * width),
        ),
    )(*blocks, gate_mat, up_mat, down_mat)


def added(*parts):
    return sum(part.astype(jnp.float32) for part in parts).astype(jnp.bfloat16)


def exchange(rows, experts):
    count, width = rows.shape
    lanes = 128
    view = rows.reshape(experts, count * width // (experts * lanes), lanes)
    view = lax.all_to_all(view, "ep", split_axis=0, concat_axis=0, tiled=True)
    return view.reshape(count, width)


def body(
    mix_tokens,
    mix_gain,
    query_weight,
    key_weight,
    value_weight,
    query_gain,
    key_gain,
    sink_logits,
    out_weight,
    moe_tokens,
    moe_gain,
    routes,
    route_logits,
    gate_weight,
    up_weight,
    down_weight,
):
    mix_out = attention(
        mix_tokens,
        mix_gain,
        query_weight,
        key_weight,
        value_weight,
        query_gain,
        key_gain,
        sink_logits,
        out_weight,
    )
    moe_rows = moe_tokens.shape[0]
    experts = lax.axis_size("ep")
    capacity = (9 * moe_rows * routes.shape[1] + 8 * experts - 1) // (8 * experts)
    moe_normed = rms_scale(moe_tokens, moe_gain).astype(jnp.bfloat16)
    targets = route_slots(routes, experts, capacity)
    slot_ids = jnp.arange(experts * capacity, dtype=jnp.int32)
    pick_rows = jnp.sum(
        (targets[None, :, :] == slot_ids[:, None, None]).astype(jnp.bfloat16), axis=2
    )
    packed = jnp.dot(pick_rows, moe_normed, preferred_element_type=jnp.float32).astype(jnp.bfloat16)
    own = exchange(packed, experts)

    def run(blocks):
        return expert_partial(blocks, gate_weight[0], up_weight[0], down_weight[0])

    near_a = outward(own, 1)
    own_b = core_swap(own)
    near_b = outward(own_b, 1)
    far_a = outward(near_a, 1)
    across_b = core_swap(near_a)
    across_a = core_swap(near_b)
    far_b = core_swap(far_a)

    own_part_a, own_part_b = run([own, own_b])
    near_part_a, across_part_b = run([near_a, across_b])
    near_part_b, across_part_a = run([near_b, across_a])
    far_part_a, far_part_b = run([far_a, far_b])

    back_a = added(near_part_a, core_swap(across_part_b))
    back_b = added(near_part_b, core_swap(across_part_a))
    far_sum = added(far_part_a, core_swap(far_part_b))
    home_b = outward(back_b, -1)
    passing = outward(far_sum, -1)
    home_a = outward(added(back_a, passing), -1)
    crossing = core_swap(added(own_part_b, home_b))
    total = added(own_part_a, home_a, crossing)
    results = exchange(total, experts)

    gate_probs = jax.nn.softmax(route_logits, axis=-1).astype(jnp.bfloat16)
    combine = jnp.where(
        targets[:, :, None] == slot_ids[None, None, :],
        gate_probs[:, :, None],
        jnp.zeros((), jnp.bfloat16),
    )
    combine = jnp.sum(combine, axis=1)
    moe_out = jnp.dot(combine, results, preferred_element_type=jnp.float32).astype(jnp.bfloat16)
    return (mix_out, moe_out)


def solution(mesh):
    placed = (
        P(("ep", "tp"), None),
        P(),
        P(),
        P(),
        P(),
        P(),
        P(),
        P(),
        P(),
        P(("ep", "tp"), None),
        P(),
        P(("ep", "tp"), None),
        P(("ep", "tp"), None),
        P("ep", None, "tp"),
        P("ep", None, "tp"),
        P("ep", "tp", None),
    )

    return jax.shard_map(
        body,
        mesh=mesh,
        in_specs=placed,
        out_specs=(P(("ep", "tp"), None), P(("ep", "tp"), None)),
        check_vma=False,
    )
```

```python
import functools

import jax
import jax.numpy as jnp
from jax import lax
from jax.experimental import pallas as pl
from jax.experimental.pallas import tpu as pltpu
from jax.sharding import PartitionSpec as P

WINDOW = 128
CORES = 2
TILE = 512


epsilon = 1e-06


def passed_along(block, axis, distance):
    devices = range(lax.axis_size(axis))
    route = [(i - distance, i) for i in devices if i - distance in devices]
    return lax.ppermute(block, axis, route)


def outward(block, distance):
    size = lax.axis_size("tp")
    route = [(i, (i + CORES * distance * (1 - 2 * (i % CORES))) % size) for i in range(size)]
    return lax.ppermute(block, "tp", route)


def core_swap(block):
    route = [(i, i ^ 1) for i in range(lax.axis_size("tp"))]
    return lax.ppermute(block, "tp", route)


def rms_scale(values, gain_vec):
    values = values.astype(jnp.float32)
    return (
        values * lax.rsqrt(jnp.mean(values * values, axis=-1, keepdims=True) + epsilon) * gain_vec
    )


def pack_kernel(capacity, *refs):
    sources, (packed_ref, targets_ref) = refs[:3], refs[3:5]
    tokens_ref, gain_ref, routes_ref = held = refs[5:8]
    copies = [
        pltpu.make_async_copy(source, place, refs[8].at[n])
        for n, (source, place) in enumerate(zip(sources, held))
    ]
    for copy in copies:
        copy.start()
    for copy in copies:
        copy.wait()
    experts = packed_ref.shape[0] // capacity
    count = tokens_ref.shape[0]
    values = tokens_ref[...].astype(jnp.float32)
    scale = lax.rsqrt(jnp.mean(values * values, axis=-1, keepdims=True) + epsilon)
    normed = (values * scale * gain_ref[...]).astype(jnp.bfloat16)
    expert_ids = lax.broadcasted_iota(jnp.int32, (experts, count), 0)
    named_by = [expert_ids == routes_ref[k : k + 1, :] for k in range(routes_ref.shape[0])]
    routed = functools.reduce(jnp.logical_or, named_by).astype(jnp.float32)
    earlier = lax.broadcasted_iota(jnp.int32, (count, count), 0) < lax.broadcasted_iota(
        jnp.int32, (count, count), 1
    )
    slots = jnp.dot(
        routed.astype(jnp.bfloat16),
        earlier.astype(jnp.float32).astype(jnp.bfloat16),
        preferred_element_type=jnp.float32,
    )
    for k, mask in enumerate(named_by):
        places = slots + (expert_ids * capacity).astype(jnp.float32)
        targets_ref[k : k + 1, :] = jnp.sum(
            jnp.where(mask, places, 0.0), axis=0, keepdims=True
        ).astype(jnp.int32)
    rows = packed_ref.shape[0]
    lows = lax.broadcasted_iota(jnp.int32, (rows, experts), 1) * capacity
    row_ids = lax.broadcasted_iota(jnp.int32, (rows, experts), 0)
    owner = (row_ids >= lows) & (row_ids < lows + capacity)
    spread = jnp.dot(
        owner.astype(jnp.float32).astype(jnp.bfloat16),
        (routed * (slots + 1.0)).astype(jnp.bfloat16),
        preferred_element_type=jnp.float32,
    )
    wanted = jnp.sum(jnp.where(owner, row_ids - lows + 1, 0).astype(jnp.float32), axis=1)
    pick = (spread == wanted[:, None]).astype(jnp.float32).astype(jnp.bfloat16)
    packed_ref[...] = jnp.dot(pick, normed, preferred_element_type=jnp.float32).astype(
        jnp.bfloat16
    )


def packed_rows(tokens, gain_vec, routes, experts, capacity):
    near = pl.BlockSpec(memory_space=pltpu.VMEM)
    width = tokens.shape[1]
    packed, targets = pl.pallas_call(
        functools.partial(pack_kernel, capacity),
        out_shape=[
            jax.ShapeDtypeStruct((experts * capacity, width), jnp.bfloat16),
            jax.ShapeDtypeStruct(routes.shape[::-1], jnp.int32),
        ],
        in_specs=[pl.BlockSpec(memory_space=pl.ANY)] * 3,
        out_specs=[near] * 2,
        scratch_shapes=[
            pltpu.VMEM(tokens.shape, tokens.dtype),
            pltpu.VMEM((1, width), gain_vec.dtype),
            pltpu.VMEM(routes.shape[::-1], routes.dtype),
            pltpu.SemaphoreType.DMA((3,)),
        ],
        compiler_params=pltpu.CompilerParams(vmem_limit_bytes=16 << 20),
    )(tokens, gain_vec.reshape(1, width), routes.T)
    return packed, targets.T


def window_attention(queries, key_ext, value_ext, sink_logits, first_pos):
    row_count = queries.shape[0]
    window_rows = key_ext.shape[0] - row_count
    blocks = row_count // window_rows
    kv_heads = key_ext.shape[1]
    group_size = queries.shape[1] // kv_heads
    head_dim = queries.shape[2]
    query_blk = queries.reshape(blocks, window_rows, kv_heads, group_size, head_dim)

    def pair_up(source):
        lower = source[:row_count].reshape(blocks, window_rows, kv_heads, head_dim)
        upper = source[window_rows:].reshape(blocks, window_rows, kv_heads, head_dim)
        return jnp.concatenate([lower, upper], axis=1)

    key_blk = pair_up(key_ext)
    value_blk = pair_up(value_ext)
    scores = jnp.einsum(
        "bqkgd,bskd->bkgqs", query_blk, key_blk, preferred_element_type=jnp.float32
    ) * head_dim ** (-0.5)
    query_pos = jnp.arange(window_rows, dtype=jnp.int32)[:, None] + window_rows
    key_pos = jnp.arange(2 * window_rows, dtype=jnp.int32)[None, :]
    pos_gap = query_pos - key_pos
    block_start = first_pos + jnp.arange(blocks, dtype=jnp.int32) * window_rows - window_rows
    key_global = block_start[:, None] + jnp.arange(2 * window_rows, dtype=jnp.int32)[None, :]
    visible = ((pos_gap >= 0) & (pos_gap <= window_rows))[None] & (key_global >= 0)[:, None, :]
    scores = jnp.where(visible[:, None, None], scores, -jnp.inf)
    sink_col = sink_logits.reshape(kv_heads, group_size)[None, :, :, None, None]
    row_top = jnp.maximum(jnp.max(scores, axis=-1, keepdims=True), sink_col)
    weights = jnp.exp(scores - row_top)
    denom_sum = jnp.sum(weights, axis=-1, keepdims=True) + jnp.exp(sink_col - row_top)
    attn_prob = (weights / denom_sum).astype(jnp.bfloat16)
    mixed_out = jnp.einsum(
        "bkgqs,bskd->bqkgd", attn_prob, value_blk, preferred_element_type=jnp.float32
    )
    return mixed_out.astype(jnp.bfloat16).reshape(row_count, -1)


def attention(
    mix_tokens,
    mix_gain,
    query_weight,
    key_weight,
    value_weight,
    query_gain,
    key_gain,
    sink_logits,
    out_weight,
):
    row_count = mix_tokens.shape[0]
    head_count = sink_logits.shape[0]
    head_dim = query_gain.shape[0]
    kv_heads = key_weight.shape[1] // head_dim
    normed = rms_scale(mix_tokens, mix_gain).astype(jnp.bfloat16)
    key_rows = jnp.dot(normed, key_weight, preferred_element_type=jnp.float32)
    key_rows = rms_scale(key_rows.reshape(row_count, kv_heads, head_dim), key_gain).astype(
        jnp.bfloat16
    )
    values = jnp.dot(normed, value_weight, preferred_element_type=jnp.float32).astype(
        jnp.bfloat16
    )
    values = values.reshape(row_count, kv_heads, head_dim)
    edge = jnp.concatenate([key_rows[row_count - WINDOW :], values[row_count - WINDOW :]], axis=1)
    rim = passed_along(edge, ("ep", "tp"), 1)
    rim_keys, rim_values = rim[:, :kv_heads], rim[:, kv_heads:]
    queries = jnp.dot(normed, query_weight, preferred_element_type=jnp.float32)
    queries = rms_scale(queries.reshape(row_count, head_count, head_dim), query_gain).astype(
        jnp.bfloat16
    )
    key_ext = jnp.concatenate([rim_keys, key_rows], axis=0)
    value_ext = jnp.concatenate([rim_values, values], axis=0)
    first_pos = lax.axis_index(("ep", "tp")) * row_count
    attended = window_attention(queries, key_ext, value_ext, sink_logits, first_pos)
    return jnp.dot(attended, out_weight, preferred_element_type=jnp.float32).astype(
        jnp.bfloat16
    )


def expert_kernel(count, *refs):
    rows = refs[:count]
    gate_ref, up_ref, down_ref = refs[count : count + 3]
    outs = refs[count + 3 : 2 * count + 3]
    stacked, hidden = refs[2 * count + 3 :]
    inner = gate_ref.shape[1]
    for k in range(count):
        stacked[k] = rows[k][...]

    @pl.loop(0, count)
    def _(k):
        block = stacked[k]
        for low in range(0, inner, TILE):
            cut = slice(low, min(low + TILE, inner))
            gate_act = jnp.dot(block, gate_ref[:, cut], preferred_element_type=jnp.float32)
            up_act = jnp.dot(block, up_ref[:, cut], preferred_element_type=jnp.float32)
            hidden[k, :, cut] = (gate_act * jax.nn.sigmoid(gate_act) * up_act).astype(
                jnp.bfloat16
            )

    @pl.loop(0, down_ref.shape[1] // TILE)
    def _(index):
        cut = pl.ds(pl.multiple_of(index * TILE, TILE), TILE)
        for k in range(count):
            outs[k][:, cut] = jnp.dot(
                hidden[k], down_ref[:, cut], preferred_element_type=jnp.float32
            ).astype(jnp.bfloat16)


def expert_partial(blocks, gate_mat, up_mat, down_mat):
    count = len(blocks)
    rows, width = blocks[0].shape
    inner = gate_mat.shape[1]
    near = pl.BlockSpec(memory_space=pltpu.VMEM)
    return pl.pallas_call(
        functools.partial(expert_kernel, count),
        out_shape=[jax.ShapeDtypeStruct((rows, width), jnp.bfloat16)] * count,
        in_specs=[near] * (count + 3),
        out_specs=[near] * count,
        scratch_shapes=[
            pltpu.VMEM((count, rows, width), jnp.bfloat16),
            pltpu.VMEM((count, rows, inner), jnp.bfloat16),
        ],
        compiler_params=pltpu.CompilerParams(vmem_limit_bytes=24 << 20),
        cost_estimate=pl.CostEstimate(
            flops=6 * count * rows * width * inner,
            transcendentals=count * rows * inner,
            bytes_accessed=2 * (3 * width * inner + 2 * count * rows * width),
        ),
    )(*blocks, gate_mat, up_mat, down_mat)


def add_kernel(*refs):
    total = refs[0][...].astype(jnp.float32)
    for ref in refs[1:-1]:
        total = total + ref[...].astype(jnp.float32)
    refs[-1][...] = total.astype(refs[-1].dtype)


def added(*parts):
    near = pl.BlockSpec(memory_space=pltpu.VMEM)
    return pl.pallas_call(
        add_kernel,
        out_shape=jax.ShapeDtypeStruct(parts[0].shape, parts[0].dtype),
        in_specs=[near] * len(parts),
        out_specs=near,
        compiler_params=pltpu.CompilerParams(vmem_limit_bytes=12 << 20),
    )(*parts)


def exchange(rows, experts):
    count, width = rows.shape
    lanes = 128
    view = rows.reshape(experts, count * width // (experts * lanes), lanes)
    view = lax.all_to_all(view, "ep", split_axis=0, concat_axis=0, tiled=True)
    return view.reshape(count, width)


def body(
    mix_tokens,
    mix_gain,
    query_weight,
    key_weight,
    value_weight,
    query_gain,
    key_gain,
    sink_logits,
    out_weight,
    moe_tokens,
    moe_gain,
    routes,
    route_logits,
    gate_weight,
    up_weight,
    down_weight,
):
    mix_out = attention(
        mix_tokens,
        mix_gain,
        query_weight,
        key_weight,
        value_weight,
        query_gain,
        key_gain,
        sink_logits,
        out_weight,
    )
    moe_rows = moe_tokens.shape[0]
    experts = lax.axis_size("ep")
    capacity = (9 * moe_rows * routes.shape[1] + 8 * experts - 1) // (8 * experts)
    packed, targets = packed_rows(moe_tokens, moe_gain, routes, experts, capacity)
    slot_ids = jnp.arange(experts * capacity, dtype=jnp.int32)
    own = exchange(packed, experts)

    def run(blocks):
        return expert_partial(blocks, gate_weight[0], up_weight[0], down_weight[0])

    near_a = outward(own, 1)
    own_b = core_swap(own)
    near_b = outward(own_b, 1)
    far_a = outward(near_a, 1)
    across_b = core_swap(near_a)
    across_a = core_swap(near_b)
    far_b = core_swap(far_a)

    (own_part_a,) = run([own])
    (own_part_b,) = run([own_b])
    near_part_a, across_part_b = run([near_a, across_b])
    (near_part_b,) = run([near_b])
    (across_part_a,) = run([across_a])
    (far_part_a,) = run([far_a])
    (far_part_b,) = run([far_b])

    back_a = added(near_part_a, core_swap(across_part_b))
    back_b = added(near_part_b, core_swap(across_part_a))
    far_sum = added(far_part_a, core_swap(far_part_b))
    home_b = outward(back_b, -1)
    passing = outward(far_sum, -1)
    home_a = outward(added(back_a, passing), -1)
    crossing = core_swap(added(own_part_b, home_b))
    total = added(own_part_a, home_a, crossing)
    results = exchange(total, experts)

    gate_probs = jax.nn.softmax(route_logits, axis=-1).astype(jnp.bfloat16)
    combine = jnp.where(
        targets[:, :, None] == slot_ids[None, None, :],
        gate_probs[:, :, None],
        jnp.zeros((), jnp.bfloat16),
    )
    combine = jnp.sum(combine, axis=1)
    moe_out = jnp.dot(combine, results, preferred_element_type=jnp.float32).astype(jnp.bfloat16)
    return (mix_out, moe_out)


def solution(mesh):
    placed = (
        P(("ep", "tp"), None),
        P(),
        P(),
        P(),
        P(),
        P(),
        P(),
        P(),
        P(),
        P(("ep", "tp"), None),
        P(),
        P(("ep", "tp"), None),
        P(("ep", "tp"), None),
        P("ep", None, "tp"),
        P("ep", None, "tp"),
        P("ep", "tp", None),
    )

    return jax.shard_map(
        body,
        mesh=mesh,
        in_specs=placed,
        out_specs=(P(("ep", "tp"), None), P(("ep", "tp"), None)),
        check_vma=False,
    )
```

```python
import functools

import jax
import jax.numpy as jnp
from jax import lax
from jax.experimental import pallas as pl
from jax.experimental.pallas import tpu as pltpu
from jax.sharding import PartitionSpec as P

WINDOW = 128
CORES = 2
TILE = 512


epsilon = 1e-06


def passed_along(block, axis, distance):
    devices = range(lax.axis_size(axis))
    route = [(i - distance, i) for i in devices if i - distance in devices]
    return lax.ppermute(block, axis, route)


def outward(block, distance):
    size = lax.axis_size("tp")
    route = [(i, (i + CORES * distance * (1 - 2 * (i % CORES))) % size) for i in range(size)]
    return lax.ppermute(block, "tp", route)


def core_swap(block):
    route = [(i, i ^ 1) for i in range(lax.axis_size("tp"))]
    return lax.ppermute(block, "tp", route)


def rms_scale(values, gain_vec):
    values = values.astype(jnp.float32)
    return (
        values * lax.rsqrt(jnp.mean(values * values, axis=-1, keepdims=True) + epsilon) * gain_vec
    )


def pack_kernel(capacity, *refs):
    sources, (packed_ref, targets_ref) = refs[:3], refs[3:5]
    tokens_ref, gain_ref, routes_ref = held = refs[5:8]
    copies = [
        pltpu.make_async_copy(source, place, refs[8].at[n])
        for n, (source, place) in enumerate(zip(sources, held))
    ]
    for copy in copies:
        copy.start()
    for copy in copies:
        copy.wait()
    experts = packed_ref.shape[0] // capacity
    count = tokens_ref.shape[0]
    values = tokens_ref[...].astype(jnp.float32)
    scale = lax.rsqrt(jnp.mean(values * values, axis=-1, keepdims=True) + epsilon)
    normed = (values * scale * gain_ref[...]).astype(jnp.bfloat16)
    expert_ids = lax.broadcasted_iota(jnp.int32, (experts, count), 0)
    named_by = [expert_ids == routes_ref[k : k + 1, :] for k in range(routes_ref.shape[0])]
    routed = functools.reduce(jnp.logical_or, named_by).astype(jnp.float32)
    earlier = lax.broadcasted_iota(jnp.int32, (count, count), 0) < lax.broadcasted_iota(
        jnp.int32, (count, count), 1
    )
    slots = jnp.dot(
        routed.astype(jnp.bfloat16),
        earlier.astype(jnp.float32).astype(jnp.bfloat16),
        preferred_element_type=jnp.float32,
    )
    for k, mask in enumerate(named_by):
        places = slots + (expert_ids * capacity).astype(jnp.float32)
        targets_ref[k : k + 1, :] = jnp.sum(
            jnp.where(mask, places, 0.0), axis=0, keepdims=True
        ).astype(jnp.int32)
    rows = packed_ref.shape[0]
    lows = lax.broadcasted_iota(jnp.int32, (rows, experts), 1) * capacity
    row_ids = lax.broadcasted_iota(jnp.int32, (rows, experts), 0)
    owner = (row_ids >= lows) & (row_ids < lows + capacity)
    spread = jnp.dot(
        owner.astype(jnp.float32).astype(jnp.bfloat16),
        (routed * (slots + 1.0)).astype(jnp.bfloat16),
        preferred_element_type=jnp.float32,
    )
    wanted = jnp.sum(jnp.where(owner, row_ids - lows + 1, 0).astype(jnp.float32), axis=1)
    pick = (spread == wanted[:, None]).astype(jnp.float32).astype(jnp.bfloat16)
    packed_ref[...] = jnp.dot(pick, normed, preferred_element_type=jnp.float32).astype(
        jnp.bfloat16
    )


def packed_rows(tokens, gain_vec, routes, experts, capacity):
    near = pl.BlockSpec(memory_space=pltpu.VMEM)
    width = tokens.shape[1]
    packed, targets = pl.pallas_call(
        functools.partial(pack_kernel, capacity),
        out_shape=[
            jax.ShapeDtypeStruct((experts * capacity, width), jnp.bfloat16),
            jax.ShapeDtypeStruct(routes.shape[::-1], jnp.int32),
        ],
        in_specs=[pl.BlockSpec(memory_space=pl.ANY)] * 3,
        out_specs=[near] * 2,
        scratch_shapes=[
            pltpu.VMEM(tokens.shape, tokens.dtype),
            pltpu.VMEM((1, width), gain_vec.dtype),
            pltpu.VMEM(routes.shape[::-1], routes.dtype),
            pltpu.SemaphoreType.DMA((3,)),
        ],
        compiler_params=pltpu.CompilerParams(vmem_limit_bytes=16 << 20),
    )(tokens, gain_vec.reshape(1, width), routes.T)
    return packed, targets.T


def window_attention(queries, key_ext, value_ext, sink_logits, first_pos):
    row_count = queries.shape[0]
    window_rows = key_ext.shape[0] - row_count
    blocks = row_count // window_rows
    kv_heads = key_ext.shape[1]
    group_size = queries.shape[1] // kv_heads
    head_dim = queries.shape[2]
    query_blk = queries.reshape(blocks, window_rows, kv_heads, group_size, head_dim)

    def pair_up(source):
        lower = source[:row_count].reshape(blocks, window_rows, kv_heads, head_dim)
        upper = source[window_rows:].reshape(blocks, window_rows, kv_heads, head_dim)
        return jnp.concatenate([lower, upper], axis=1)

    key_blk = pair_up(key_ext)
    value_blk = pair_up(value_ext)
    scores = jnp.einsum(
        "bqkgd,bskd->bkgqs", query_blk, key_blk, preferred_element_type=jnp.float32
    ) * head_dim ** (-0.5)
    query_pos = jnp.arange(window_rows, dtype=jnp.int32)[:, None] + window_rows
    key_pos = jnp.arange(2 * window_rows, dtype=jnp.int32)[None, :]
    pos_gap = query_pos - key_pos
    block_start = first_pos + jnp.arange(blocks, dtype=jnp.int32) * window_rows - window_rows
    key_global = block_start[:, None] + jnp.arange(2 * window_rows, dtype=jnp.int32)[None, :]
    visible = ((pos_gap >= 0) & (pos_gap <= window_rows))[None] & (key_global >= 0)[:, None, :]
    scores = jnp.where(visible[:, None, None], scores, -jnp.inf)
    sink_col = sink_logits.reshape(kv_heads, group_size)[None, :, :, None, None]
    row_top = jnp.maximum(jnp.max(scores, axis=-1, keepdims=True), sink_col)
    weights = jnp.exp(scores - row_top)
    denom_sum = jnp.sum(weights, axis=-1, keepdims=True) + jnp.exp(sink_col - row_top)
    attn_prob = (weights / denom_sum).astype(jnp.bfloat16)
    mixed_out = jnp.einsum(
        "bkgqs,bskd->bqkgd", attn_prob, value_blk, preferred_element_type=jnp.float32
    )
    return mixed_out.astype(jnp.bfloat16).reshape(row_count, -1)


def attention(
    mix_tokens,
    mix_gain,
    query_weight,
    key_weight,
    value_weight,
    query_gain,
    key_gain,
    sink_logits,
    out_weight,
):
    row_count = mix_tokens.shape[0]
    head_count = sink_logits.shape[0]
    head_dim = query_gain.shape[0]
    kv_heads = key_weight.shape[1] // head_dim
    normed = rms_scale(mix_tokens, mix_gain).astype(jnp.bfloat16)
    key_rows = jnp.dot(normed, key_weight, preferred_element_type=jnp.float32)
    key_rows = rms_scale(key_rows.reshape(row_count, kv_heads, head_dim), key_gain).astype(
        jnp.bfloat16
    )
    values = jnp.dot(normed, value_weight, preferred_element_type=jnp.float32).astype(
        jnp.bfloat16
    )
    values = values.reshape(row_count, kv_heads, head_dim)
    edge = jnp.concatenate([key_rows[row_count - WINDOW :], values[row_count - WINDOW :]], axis=1)
    rim = passed_along(edge, ("ep", "tp"), 1)
    rim_keys, rim_values = rim[:, :kv_heads], rim[:, kv_heads:]
    queries = jnp.dot(normed, query_weight, preferred_element_type=jnp.float32)
    queries = rms_scale(queries.reshape(row_count, head_count, head_dim), query_gain).astype(
        jnp.bfloat16
    )
    key_ext = jnp.concatenate([rim_keys, key_rows], axis=0)
    value_ext = jnp.concatenate([rim_values, values], axis=0)
    first_pos = lax.axis_index(("ep", "tp")) * row_count
    attended = window_attention(queries, key_ext, value_ext, sink_logits, first_pos)
    return jnp.dot(attended, out_weight, preferred_element_type=jnp.float32).astype(
        jnp.bfloat16
    )


def expert_kernel(count, *refs):
    rows = refs[:count]
    gate_ref, up_ref, down_ref = refs[count : count + 3]
    outs = refs[count + 3 : 2 * count + 3]
    stacked, hidden = refs[2 * count + 3 :]
    inner = gate_ref.shape[1]
    for k in range(count):
        stacked[k] = rows[k][...]

    @pl.loop(0, count)
    def _(k):
        block = stacked[k]
        for low in range(0, inner, TILE):
            cut = slice(low, min(low + TILE, inner))
            gate_act = jnp.dot(block, gate_ref[:, cut], preferred_element_type=jnp.float32)
            up_act = jnp.dot(block, up_ref[:, cut], preferred_element_type=jnp.float32)
            hidden[k, :, cut] = (gate_act * jax.nn.sigmoid(gate_act) * up_act).astype(
                jnp.bfloat16
            )

    @pl.loop(0, down_ref.shape[1] // TILE)
    def _(index):
        cut = pl.ds(pl.multiple_of(index * TILE, TILE), TILE)
        for k in range(count):
            outs[k][:, cut] = jnp.dot(
                hidden[k], down_ref[:, cut], preferred_element_type=jnp.float32
            ).astype(jnp.bfloat16)


def expert_partial(blocks, gate_mat, up_mat, down_mat):
    count = len(blocks)
    rows, width = blocks[0].shape
    inner = gate_mat.shape[1]
    near = pl.BlockSpec(memory_space=pltpu.VMEM)
    return pl.pallas_call(
        functools.partial(expert_kernel, count),
        out_shape=[jax.ShapeDtypeStruct((rows, width), jnp.bfloat16)] * count,
        in_specs=[near] * (count + 3),
        out_specs=[near] * count,
        scratch_shapes=[
            pltpu.VMEM((count, rows, width), jnp.bfloat16),
            pltpu.VMEM((count, rows, inner), jnp.bfloat16),
        ],
        compiler_params=pltpu.CompilerParams(vmem_limit_bytes=24 << 20),
        cost_estimate=pl.CostEstimate(
            flops=6 * count * rows * width * inner,
            transcendentals=count * rows * inner,
            bytes_accessed=2 * (3 * width * inner + 2 * count * rows * width),
        ),
    )(*blocks, gate_mat, up_mat, down_mat)


def add_kernel(*refs):
    total = refs[0][...].astype(jnp.float32)
    for ref in refs[1:-1]:
        total = total + ref[...].astype(jnp.float32)
    refs[-1][...] = total.astype(refs[-1].dtype)


def added(*parts):
    near = pl.BlockSpec(memory_space=pltpu.VMEM)
    return pl.pallas_call(
        add_kernel,
        out_shape=jax.ShapeDtypeStruct(parts[0].shape, parts[0].dtype),
        in_specs=[near] * len(parts),
        out_specs=near,
        compiler_params=pltpu.CompilerParams(vmem_limit_bytes=12 << 20),
    )(*parts)


def part_kernel(whole_ref, first_ref, second_ref):
    count = first_ref.shape[0]
    first_ref[...] = whole_ref[:count]
    second_ref[...] = whole_ref[count:]


def parted(whole):
    near = pl.BlockSpec(memory_space=pltpu.VMEM)
    return pl.pallas_call(
        part_kernel,
        out_shape=[jax.ShapeDtypeStruct((whole.shape[0] // 2, whole.shape[1]), whole.dtype)] * 2,
        in_specs=[near],
        out_specs=[near] * 2,
        compiler_params=pltpu.CompilerParams(vmem_limit_bytes=12 << 20),
    )(whole)


def join_kernel(first_ref, second_ref, whole_ref):
    count = first_ref.shape[0]
    whole_ref[:count] = first_ref[...]
    whole_ref[count:] = second_ref[...]


def joined(first, second):
    near = pl.BlockSpec(memory_space=pltpu.VMEM)
    return pl.pallas_call(
        join_kernel,
        out_shape=jax.ShapeDtypeStruct(
            (first.shape[0] + second.shape[0], first.shape[1]), first.dtype
        ),
        in_specs=[near] * 2,
        out_specs=near,
        compiler_params=pltpu.CompilerParams(vmem_limit_bytes=12 << 20),
    )(first, second)


def exchange(rows, experts):
    count, width = rows.shape
    lanes = 128
    view = rows.reshape(experts, count * width // (experts * lanes), lanes)
    view = lax.all_to_all(view, "ep", split_axis=0, concat_axis=0, tiled=True)
    return view.reshape(count, width)


def body(
    mix_tokens,
    mix_gain,
    query_weight,
    key_weight,
    value_weight,
    query_gain,
    key_gain,
    sink_logits,
    out_weight,
    moe_tokens,
    moe_gain,
    routes,
    route_logits,
    gate_weight,
    up_weight,
    down_weight,
):
    mix_out = attention(
        mix_tokens,
        mix_gain,
        query_weight,
        key_weight,
        value_weight,
        query_gain,
        key_gain,
        sink_logits,
        out_weight,
    )
    moe_rows = moe_tokens.shape[0]
    experts = lax.axis_size("ep")
    capacity = (9 * moe_rows * routes.shape[1] + 8 * experts - 1) // (8 * experts)
    packed, targets = packed_rows(moe_tokens, moe_gain, routes, experts, capacity)
    slot_ids = jnp.arange(experts * capacity, dtype=jnp.int32)
    own = exchange(packed, experts)

    def run(blocks):
        return expert_partial(blocks, gate_weight[0], up_weight[0], down_weight[0])

    near_parts = [outward(part, 1) for part in parted(own)]
    far_parts = [outward(part, 1) for part in near_parts]
    near_a = joined(*near_parts)
    far_a = joined(*far_parts)
    own_b = core_swap(own)
    near_b = outward(own_b, 1)
    across_b = core_swap(near_a)
    across_a = core_swap(near_b)
    far_b = core_swap(far_a)

    (own_part_a,) = run([own])
    (own_part_b,) = run([own_b])
    near_part_a, across_part_b = run([near_a, across_b])
    (near_part_b,) = run([near_b])
    (across_part_a,) = run([across_a])
    (far_part_a,) = run([far_a])
    (far_part_b,) = run([far_b])

    back_a = added(near_part_a, core_swap(across_part_b))
    back_b = added(near_part_b, core_swap(across_part_a))
    far_sum = added(far_part_a, core_swap(far_part_b))
    home_b = outward(back_b, -1)
    passing = outward(far_sum, -1)
    home_a = outward(added(back_a, passing), -1)
    crossing = core_swap(added(own_part_b, home_b))
    settled = added(own_part_a, crossing)
    total = added(settled, home_a)
    results = exchange(total, experts)

    gate_probs = jax.nn.softmax(route_logits, axis=-1).astype(jnp.bfloat16)
    combine = jnp.where(
        targets[:, :, None] == slot_ids[None, None, :],
        gate_probs[:, :, None],
        jnp.zeros((), jnp.bfloat16),
    )
    combine = jnp.sum(combine, axis=1)
    moe_out = jnp.dot(combine, results, preferred_element_type=jnp.float32).astype(jnp.bfloat16)
    return (mix_out, moe_out)


def solution(mesh):
    placed = (
        P(("ep", "tp"), None),
        P(),
        P(),
        P(),
        P(),
        P(),
        P(),
        P(),
        P(),
        P(("ep", "tp"), None),
        P(),
        P(("ep", "tp"), None),
        P(("ep", "tp"), None),
        P("ep", None, "tp"),
        P("ep", None, "tp"),
        P("ep", "tp", None),
    )

    return jax.shard_map(
        body,
        mesh=mesh,
        in_specs=placed,
        out_specs=(P(("ep", "tp"), None), P(("ep", "tp"), None)),
        check_vma=False,
    )
```
